32 devices in a mesh: grp: 2 (over y), ra: 4 (over z), cb: 4 (over x, core).
Axes of the slice: x: 2, y: 2, z: 4, core: 2. Of those that a mesh axis runs over, the one named last changes fastest.
Arguments:
- stream: bfloat16 [256, 4096], P('grp', 'ra'), parts along dimension 0, may hold values from -180 to 180
- w_gate: float32 [2, 4096, 11264], P(None, 'ra', 'cb'), may hold values from -0.09375 to 0.09375
- w_up: float32 [2, 4096, 11264], P(None, 'ra', 'cb'), may hold values from -0.09375 to 0.09375
- w_down: float32 [2, 11264, 4096], P(None, 'cb', 'ra'), may hold values from -0.0546875 to 0.0546875
- gate_scale: float32 [2, 11264], P(None, 'cb'), may hold values from 0.5 to 2
- up_scale: float32 [2, 11264], P(None, 'cb'), may hold values from 0.5 to 2
- down_scale: float32 [2, 4096], P(None, 'ra'), may hold values from 0.5 to 2
- pre_gain: float32 [2, 4096], P(None, 'ra'), may hold values from 0.1 to 1.9
- out_gain: float32 [4096], P('ra'), may hold values from 0.1 to 1.9
Outputs:
- normed: bfloat16 [256, 4096], P('grp', 'ra'), parts along dimension 0
The draws below stay inside these ranges and needn't reach their ends.
There are 2 independent parts, one for each index of `grp`. The reference program is written for one: setup_inputs(seed, part) draws one part's arguments, and reference() takes and returns one part's arrays. A program takes and returns all parts, laid end to end along the dimension named above; an argument that names none is the same for every part. Nothing has to cross between parts.
All inputs are finite; a program needn't handle non-finite values.
Results may differ from the reference program's by a relative error of at most 0.018.
Values may be sent and summed in bfloat16 or wider, within the bound.
No kernel may reach another device: no remote copies, remote signals or barrier semaphores. Data moves between devices by JAX's collectives and lax.ppermute only.
A program may use at most 192 MiB of HBM per device.

```python
import math
import jax
import jax.numpy as jnp
from jax import lax

D = 4096
FF = 11264
LAYERS = 2
TOK = 128
N_CB = 4


def draw_stream(key, part):
    first = jax.random.fold_in(key, 11)
    second = jax.random.fold_in(key, 12)
    channel = jnp.exp(math.log(3.0) * jnp.arange(D, dtype=jnp.float32) / D)
    base = jnp.clip(jax.random.normal(first, (TOK, D), jnp.float32), -6.0, 6.0)
    rows = jnp.exp(jax.random.uniform(second, (TOK, 1), jnp.float32, 0.0, math.log(10.0)))
    return (base * rows * channel[None, :]).astype(jnp.bfloat16)


def shard_levels(key, extent, split, least, top_value):
    def one(axis_at, blocks):
        heights = jax.random.uniform(jax.random.fold_in(jax.random.fold_in(key, 6), axis_at), (blocks,), jnp.float32, least / len(split), top_value / len(split))
        return jnp.repeat(jnp.exp(heights), extent[axis_at] // blocks).reshape((-1,) + (1,) * (len(extent) - axis_at - 1))

    factor_of = one(*split[0])
    for cut in split[1:]:
        factor_of = factor_of * one(*cut)
    return factor_of


def gaussian(rng, extent, width, most, cuts=(), held_as=jnp.bfloat16):
    level = shard_levels(rng, extent, cuts, -0.22, 0.18) if cuts else 1.0
    array = jax.random.normal(rng, extent, jnp.float32) * width * level
    return jnp.minimum(jnp.maximum(array, -most), most).astype(held_as)


def setup_inputs(seed: int = 0, part: int = 0) -> dict:
    splits = jax.random.split(jax.random.key(seed), 10)
    part_splits = jax.random.split(jax.random.fold_in(splits[9], part), 10)
    stream = draw_stream(jax.random.fold_in(jax.random.fold_in(splits[9], part), 71), part)
    w_gate = gaussian(splits[1], (LAYERS, D, FF), D ** -0.5, 0.09375, ((1, 4), (2, 4)), jnp.float32)
    w_up = gaussian(splits[2], (LAYERS, D, FF), D ** -0.5, 0.09375, ((1, 4), (2, 4)), jnp.float32)
    w_down = gaussian(splits[3], (LAYERS, FF, D), FF ** -0.5, 0.0546875, ((1, 4), (2, 4)), jnp.float32)
    gate_scale = jnp.clip(jnp.exp(math.log(2.0) - 1.3862944 * jax.random.uniform(splits[4], (LAYERS, FF), jnp.float32) ** shard_levels(splits[4], (LAYERS, FF), ((1, 4),), -0.2, 0.2)), 0.5, 2.0)
    up_scale = jnp.clip(jnp.exp(math.log(2.0) - 1.3862944 * jax.random.uniform(splits[5], (LAYERS, FF), jnp.float32) ** shard_levels(splits[5], (LAYERS, FF), ((1, 4),), -0.2, 0.2)), 0.5, 2.0)
    down_scale = jnp.clip(jnp.exp(math.log(2.0) - 1.3862944 * jax.random.uniform(splits[6], (LAYERS, D), jnp.float32) ** shard_levels(splits[6], (LAYERS, D), ((1, 4),), -0.2, 0.2)), 0.5, 2.0)
    pre_gain = jnp.clip(1.0 + 0.18 * jax.random.normal(splits[7], (LAYERS, D), jnp.float32), 0.1, 1.9)
    out_gain = jnp.clip(1.0 + 0.18 * jax.random.normal(splits[8], (D,), jnp.float32), 0.1, 1.9)
    return dict(stream=stream, w_gate=w_gate, w_up=w_up, w_down=w_down, gate_scale=gate_scale, up_scale=up_scale, down_scale=down_scale, pre_gain=pre_gain, out_gain=out_gain)


def reference(stream, w_gate, w_up, w_down, gate_scale, up_scale, down_scale, pre_gain, out_gain):
    current = stream
    for layer in range(LAYERS):
        xvals = lax.optimization_barrier(current).astype(jnp.float32)
        rinv = lax.rsqrt(lax.optimization_barrier(jnp.mean(xvals * xvals, axis=1, keepdims=True)) + 1e-06)
        scaled = (xvals * pre_gain[layer]).astype(jnp.bfloat16)
        gate = jnp.dot(scaled, w_gate[layer].astype(jnp.bfloat16), preferred_element_type=jnp.float32) * rinv * gate_scale[layer]
        upper = jnp.dot(scaled, w_up[layer].astype(jnp.bfloat16), preferred_element_type=jnp.float32) * rinv * up_scale[layer]
        hidden = (jax.nn.silu(gate) * upper).astype(jnp.bfloat16)
        blocks = hidden.astype(jnp.float32).reshape(TOK, N_CB, FF // N_CB)
        down_blocks = w_down[layer].astype(jnp.bfloat16).astype(jnp.float32).reshape(N_CB, FF // N_CB, D)
        partial_value = jnp.einsum('tcf,cfd->ctd', blocks, down_blocks).astype(jnp.bfloat16)
        branch = lax.optimization_barrier(jnp.sum(partial_value.astype(jnp.float32), axis=0)) * down_scale[layer]
        current = (0.5 * xvals + branch).astype(jnp.bfloat16)
    xvals = lax.optimization_barrier(current).astype(jnp.float32)
    rinv = lax.rsqrt(lax.optimization_barrier(jnp.mean(xvals * xvals, axis=1, keepdims=True)) + 1e-06)
    return (xvals * rinv * out_gain).astype(jnp.bfloat16)
```

```python
import jax
import jax.numpy as jnp
from jax import lax
from jax.experimental import pallas as pl
from jax.experimental.pallas import tpu as pltpu
from jax.sharding import PartitionSpec as P


CHUNKS = 2
LANES = 128
BF = jnp.bfloat16
F32 = jnp.float32


def shift(value, axis, step):
    size = lax.axis_size(axis)
    return lax.ppermute(value, axis, [(i, (i + step) % size) for i in range(size)])


def swap(value, axis, bit):
    size = lax.axis_size(axis)
    return lax.ppermute(value, axis, [(i, i ^ bit) for i in range(size)])


def stages(axis):
    return [1 << s for s in range(lax.axis_size(axis).bit_length() - 1)]


def column_block(extent):
    for size in (256, 128):
        if extent % size == 0:
            return size
    return extent


def chunk_bounds(blocks):
    count = min(CHUNKS, blocks)
    edges = [-(-blocks * c // count) for c in range(count + 1)]
    return list(zip(edges[:-1], edges[1:]))


def two_floats(value):
    high = lax.reduce_precision(value, 8, 7)
    middle = lax.reduce_precision(value - high, 8, 7)
    low = value - high - middle
    lane = lax.broadcasted_iota(jnp.int32, (value.shape[0], LANES), 1)
    picked = jnp.where(lane == 0, high, jnp.where(lane == 1, middle, jnp.where(lane == 2, low, 0.0)))
    return picked.astype(BF)


def fetch(copies):
    for copy in copies:
        copy.start()
    return copies


def gate_up_kernel(x_ref, wg_hbm, wu_hbm, extra_ref, *rest, layer, lo, blk, cut, tail):
    outs, (buf, sems) = rest[:-2], rest[-2:]
    count = cut // blk
    copies = fetch(
        [
            pltpu.make_async_copy(w.at[layer, :, pl.ds((lo + j) * blk, blk)], buf.at[j, i], sems.at[j, i])
            for j in range(count)
            for i, w in enumerate((wg_hbm, wu_hbm))
        ]
    )
    rows = x_ref.shape[0] // len(outs)
    if tail:
        for i, out in enumerate(outs):
            out[:, 2 * cut :] = extra_ref[i * rows : (i + 1) * rows]
    x = x_ref[...]
    for j in range(count):
        for i in range(2):
            copies[2 * j + i].wait()
            value = jnp.dot(x, buf[j, i].astype(BF), preferred_element_type=F32).astype(BF)
            at = i * cut + j * blk
            for p, out in enumerate(outs):
                out[:, at : at + blk] = value[p * rows : (p + 1) * rows]


def gate_up(scaled, w_gate, w_up, extra, tail, layer, lo, hi, blk, pieces):
    tokens, depth = scaled.shape
    cut = (hi - lo) * blk
    rows = tokens // pieces
    wide = 2 * cut + (LANES if tail else 0)
    vmem = pl.BlockSpec(memory_space=pltpu.VMEM)
    hbm = pl.BlockSpec(memory_space=pl.ANY)
    return pl.pallas_call(
        lambda *refs: gate_up_kernel(*refs, layer=layer, lo=lo, blk=blk, cut=cut, tail=tail),
        in_specs=[vmem, hbm, hbm, vmem if tail else hbm],
        out_specs=[vmem] * pieces,
        out_shape=[jax.ShapeDtypeStruct((rows, wide), BF)] * pieces,
        scratch_shapes=[pltpu.VMEM((hi - lo, 2, depth, blk), F32), pltpu.SemaphoreType.DMA((hi - lo, 2))],
        cost_estimate=pl.CostEstimate(
            flops=4 * tokens * depth * cut, bytes_accessed=8 * depth * cut, transcendentals=0
        ),
    )(scaled, w_gate, w_up, extra)


def down_kernel(h_ref, w_hbm, *rest, layer, lo, blk, count):
    out, buf, sems = rest[-3:]
    copies = fetch(
        [
            pltpu.make_async_copy(w_hbm.at[layer, pl.ds((lo + j) * blk, blk)], buf.at[j], sems.at[j])
            for j in range(count)
        ]
    )
    total = rest[0][...] if len(rest) == 4 else None
    for j in range(count):
        copies[j].wait()
        value = jnp.dot(h_ref[:, j * blk : (j + 1) * blk], buf[j].astype(BF), preferred_element_type=F32)
        total = value if total is None else total + value
    out[...] = total.astype(out.dtype)


def down(hidden, w_down, layer, lo, hi, blk, before, dtype):
    tokens = hidden.shape[0]
    width = w_down.shape[2]
    vmem = pl.BlockSpec(memory_space=pltpu.VMEM)
    return pl.pallas_call(
        lambda *refs: down_kernel(*refs, layer=layer, lo=lo, blk=blk, count=hi - lo),
        in_specs=[vmem, pl.BlockSpec(memory_space=pl.ANY)] + ([] if before is None else [vmem]),
        out_specs=vmem,
        out_shape=jax.ShapeDtypeStruct((tokens, width), dtype),
        scratch_shapes=[pltpu.VMEM((hi - lo, blk, width), F32), pltpu.SemaphoreType.DMA((hi - lo,))],
        cost_estimate=pl.CostEstimate(
            flops=2 * tokens * width * (hi - lo) * blk,
            bytes_accessed=4 * width * (hi - lo) * blk,
            transcendentals=0,
        ),
    )(hidden, w_down, *(() if before is None else (before,)))


def ra_sum(squares):
    for bit in stages("ra"):
        squares = squares + swap(squares, "ra", bit)
    return squares


def cb_sum(mine):
    size = lax.axis_size("cb")
    if size == 1:
        return mine.astype(F32)
    pair = mine.astype(F32) + swap(mine, "cb", 1).astype(F32)
    if size == 2:
        return pair
    sent = pair.astype(BF)
    total = sent.astype(F32)
    for step in range(2, size, 2):
        total = total + shift(sent, "cb", step).astype(F32)
    return total


def local(stream, w_gate, w_up, w_down, gate_scale, up_scale, down_scale, pre_gain, out_gain):
    layers, width, ff = w_gate.shape
    tokens = stream.shape[0]
    parts = lax.axis_size("ra")
    features = width * parts
    share = tokens // parts
    bits = stages("ra")
    me = lax.axis_index("ra")
    home = sum(((me // bit) % 2) * bits[-1 - s] for s, bit in enumerate(bits))

    def reorder(value):
        if parts == 1:
            return value
        return jnp.concatenate(
            [lax.dynamic_slice_in_dim(value, (p ^ home) * share, share, 0) for p in range(parts)], axis=0
        )

    blk = column_block(ff)
    bounds = chunk_bounds(ff // blk)
    current = reorder(stream)
    for layer in range(layers):
        xvals = current.astype(F32)
        scaled = (xvals * pre_gain[layer]).astype(BF)
        extra = two_floats(jnp.sum(xvals * xvals, axis=1, keepdims=True))
        products = []
        for lo, hi in bounds:
            product = gate_up(scaled, w_gate, w_up, extra, lo == 0, layer, lo, hi, blk, 2 if bits else 1)
            products.append(product)
            extra = product[0]
        terms = None
        for (lo, hi), product in zip(bounds, products):
            cut = (hi - lo) * blk
            cols = slice(lo * blk, hi * blk)
            keep = product[0].astype(F32)
            send = product[-1]
            for s, bit in enumerate(bits):
                taken = swap(send, "ra", bit)
                keep = keep + taken.astype(F32)
                if s + 1 < len(bits):
                    half = keep.shape[0] // 2
                    send = keep[half:, : 2 * cut].astype(BF)
                    if lo == 0:
                        squares = jnp.sum(keep[half:, 2 * cut :], axis=1, keepdims=True)
                        send = jnp.concatenate([send, two_floats(squares)], axis=1)
                    keep = keep[:half]
            if lo == 0:
                total = jnp.sum(keep[:, 2 * cut :], axis=1, keepdims=True)
                rinv = lax.rsqrt(total / features + 1e-06)
            gate = keep[:, :cut] * rinv * gate_scale[layer, cols]
            upper = keep[:, cut : 2 * cut] * rinv * up_scale[layer, cols]
            hidden = (jax.nn.silu(gate) * upper).astype(BF)
            for s, bit in reversed(list(enumerate(bits))):
                taken = swap(hidden, "ra", bit)
                hidden = jnp.concatenate([hidden, taken], axis=0)
            last = hi == bounds[-1][1]
            terms = down(hidden, w_down, layer, lo, hi, blk, terms, BF if last else F32)
        branch = cb_sum(terms) * down_scale[layer]
        current = (0.5 * xvals + branch).astype(BF)
    xvals = reorder(current).astype(F32)
    final_sum = ra_sum(jnp.sum(xvals * xvals, axis=1))
    rinv = lax.rsqrt(final_sum / features + 1e-06)[:, None]
    return (xvals * rinv * out_gain).astype(BF)


def solution(mesh):
    placed = (
        P("grp", "ra"),
        P(None, "ra", "cb"),
        P(None, "ra", "cb"),
        P(None, "cb", "ra"),
        P(None, "cb"),
        P(None, "cb"),
        P(None, "ra"),
        P(None, "ra"),
        P("ra"),
    )
    return jax.shard_map(
        local, mesh=mesh, in_specs=placed, out_specs=P("grp", "ra"), check_vma=False
    )
```
